32 devices in a mesh: sp: 4 (over z), dp: 8 (over y, x, core).
Axes of the slice: x: 2, y: 2, z: 4, core: 2. Of those that a mesh axis runs over, the one named last changes fastest.
Arguments:
- value_half: bfloat16 [8, 1536, 2048], P('dp', 'sp'), may hold values from -6 to 6
- gate_half: bfloat16 [8, 1536, 2048], P('dp', 'sp'), may hold values from -9 to 9
- conv_taps: bfloat16 [31, 2048], replicated, may hold values from -1 to 1
- norm_gain: float32 [2048], replicated, may hold values from 0.1 to 1.9
- norm_shift: float32 [2048], replicated, may hold values from -3 to 3
- out_weight: bfloat16 [2048, 2048], P('dp', 'sp'), may hold values from -0.125 to 0.125
Outputs:
- module_out: bfloat16 [8, 1536, 2048], P('dp', 'sp')
The draws below stay inside these ranges and needn't reach their ends.
All inputs are finite; a program needn't handle non-finite values.
Results may differ from the reference program's by a relative error of at most 0.0064.
Values may be sent and summed in bfloat16 or wider, within the bound.
A program may use at most 64 MiB of HBM per device.

```python
import jax
import jax.numpy as jnp
from jax import lax

D = 2048
CONV_W = 31
SEQ_LEN = 1536
SEQS = 8


def steps_of(stream_key, shape, shards, least, top_value):
    factor_of, own = 1.0, jax.random.fold_in(stream_key, 6)
    for position, shards_of in shards:
        heights = jnp.exp(jax.random.uniform(jax.random.fold_in(own, position), (shards_of,), jnp.float32, least / len(shards), top_value / len(shards)))
        factor_of = factor_of * jnp.repeat(heights, shape[position] // shards_of).reshape([-1 if axis == position else 1 for axis in range(len(shape))])
    return factor_of


def noise(own_key, shape, scale, limit, pieces=(), kind=jnp.bfloat16):
    values = jax.random.normal(own_key, shape, jnp.float32) * scale
    if len(pieces) > 0:
        values = steps_of(own_key, shape, pieces, -0.22, 0.18) * values
    return jnp.clip(values, min=-limit, max=limit).astype(kind)


def setup_inputs(seed: int = 0) -> dict:
    keys = jax.random.split(jax.random.key(seed), 7)
    value_half = noise(keys[0], (SEQS, SEQ_LEN, D), 1.0, 6.0, ((0, 8), (1, 4)))
    gate_half = noise(keys[1], (SEQS, SEQ_LEN, D), 1.5, 9.0, ((0, 8), (1, 4)))
    conv_taps = noise(keys[2], (CONV_W, D), CONV_W ** -0.5, 1.0)
    norm_gain = jnp.clip(1.0 + 0.18 * jax.random.normal(keys[3], (D,), jnp.float32), 0.1, 1.9)
    norm_shift = noise(keys[4], (D,), 0.5, 3.0, (), jnp.float32)
    out_weight = noise(keys[5], (D, D), D ** -0.5, 0.125, ((0, 8), (1, 4)))
    return {"value_half": value_half, "gate_half": gate_half, "conv_taps": conv_taps, "norm_gain": norm_gain, "norm_shift": norm_shift, "out_weight": out_weight}


EPSILON = 1e-06

def causal_mix(gated, conv_taps):
    tap_count = conv_taps.shape[0]
    length = gated.shape[0]
    padded = jnp.concatenate([jnp.zeros((tap_count - 1, gated.shape[1]), gated.dtype), gated], 0)
    running = jnp.zeros((length, gated.shape[1]), jnp.float32)
    for tap_index in range(tap_count):
        running = running + padded[tap_index:tap_index + length].astype(jnp.float32) * conv_taps[tap_index].astype(jnp.float32)
    return running.astype(jnp.bfloat16)

def one_sequence(pair, conv_taps, norm_gain, norm_shift, out_weight):
    value_rows, gate_rows = pair
    gated = (value_rows.astype(jnp.float32) * jax.nn.sigmoid(gate_rows.astype(jnp.float32))).astype(jnp.bfloat16)
    convolved = causal_mix(gated, conv_taps).astype(jnp.float32)
    mean_row = lax.optimization_barrier(jnp.mean(convolved, axis=-1, keepdims=True))
    centered = convolved - mean_row
    variance = lax.optimization_barrier(jnp.mean(centered * centered, axis=-1, keepdims=True))
    normed = centered * lax.rsqrt(variance + EPSILON) * norm_gain + norm_shift
    activated = jax.nn.silu(normed).astype(jnp.bfloat16)
    return jnp.dot(activated, out_weight, preferred_element_type=jnp.float32).astype(jnp.bfloat16)

def reference(value_half, gate_half, conv_taps, norm_gain, norm_shift, out_weight):
    return lax.map(lambda pair: one_sequence(pair, conv_taps, norm_gain, norm_shift, out_weight), (value_half, gate_half))
```

```python
import math

import jax
import jax.numpy as jnp
from jax import lax
from jax.experimental import pallas as pl
from jax.experimental.pallas import tpu as pltpu
from jax.sharding import PartitionSpec as P

EPSILON = 1e-06
MESH = pl.DeviceIdType.MESH
F32 = jnp.float32
BF16 = jnp.bfloat16
LANES = 128


def half_sigmoid(x):
    return 0.5 * jnp.tanh(0.5 * x) + 0.5


def nearest(me, count, k):
    place = jnp.int32(0)
    for here in range(count):
        there = sorted(range(count), key=lambda j: (abs(j - here), j))[k]
        place = place + jnp.where(me == here, there, 0).astype(jnp.int32)
    return place


def make_kernel(sp, dp, xs, ys, parts, tok, width, taps, rows, cols, pad):
    group = sp // parts
    part_cols = group * cols
    half_rows = rows // 2
    blocks = width // LANES
    row_chunk = 128 if tok % 128 == 0 else tok
    lead = pad - (taps - 1)
    in_parts = 4 if blocks % 4 == 0 else 1
    in_cols = width // in_parts
    streamed = rows % LANES == 0

    def kernel(v_hbm, g_hbm, taps_hbm, gain_hbm, shift_hbm, w_hbm, out_hbm,
               v_in, g_in, halo_v, halo_g, taps_in, taps_f, gain, shift, gated, conv, act, acc, out_v, wall,
               in_sem, out_sem, halo_send, halo_recv, send_sem, z_sem, recv_sem):
        s = lax.axis_index("sp")
        d = lax.axis_index("dp")
        core = lax.rem(d, 2)
        x = lax.rem(d // 2, xs)
        y = d // (2 * xs)

        def index(yy, xx, cc):
            return (yy * xs + xx) * 2 + cc

        sibling = index(y, x, 1 - core)

        def along_x(step):
            return lax.rem(x + step, xs)

        def along_y(step):
            return lax.rem(y + step, ys)

        own = wall.at[pl.ds(pl.multiple_of(d * rows, rows), rows), pl.ds(pl.multiple_of(s * cols, cols), cols)]
        w_copy = pltpu.make_async_copy(w_hbm, own, in_sem.at[0])
        w_copy.start()
        loads = []
        for part in range(in_parts):
            sl = pl.ds(part * in_cols, in_cols)
            pair = (
                pltpu.make_async_copy(v_hbm.at[0, :, sl], v_in.at[:, sl], in_sem.at[4 + 2 * part]),
                pltpu.make_async_copy(g_hbm.at[0, :, sl], g_in.at[:, sl], in_sem.at[5 + 2 * part]),
            )
            loads.append(pair)
            for copy in pair:
                copy.start()
        small = [
            pltpu.make_async_copy(taps_hbm, taps_in, in_sem.at[1]),
            pltpu.make_async_copy(gain_hbm, gain, in_sem.at[2]),
            pltpu.make_async_copy(shift_hbm, shift, in_sem.at[3]),
        ]
        for copy in small:
            copy.start()

        barrier = pltpu.get_barrier_semaphore()
        friends = [(s, sibling)]
        friends += [(s, index(y, along_x(i), core)) for i in range(1, xs)]
        friends += [(s, index(along_y(i), x, core)) for i in range(1, ys)]
        friends += [(lax.rem(s + i, sp), d) for i in range(1, sp)]
        for friend in friends:
            pl.semaphore_signal(barrier, inc=1, device_id=friend, device_id_type=MESH)
        pl.semaphore_wait(barrier, len(friends))
        w_copy.wait()

        sent = []

        def send(region, sem, target):
            copy = pltpu.make_async_remote_copy(
                src_ref=region, dst_ref=region, send_sem=send_sem.at[len(sent)], recv_sem=sem,
                device_id=target, device_id_type=MESH)
            copy.start()
            sent.append(copy)

        def arrived(region, sem):
            pltpu.make_async_remote_copy(
                src_ref=region, dst_ref=region, send_sem=send_sem.at[0], recv_sem=sem,
                device_id=(s, sibling), device_id_type=MESH).wait_recv()

        def block(half, who):
            return wall.at[pl.ds(pl.multiple_of(d * rows + half * half_rows, half_rows), half_rows),
                           pl.ds(pl.multiple_of(who * cols, cols), cols)]

        def strip(half, dd, part):
            return wall.at[pl.ds(pl.multiple_of(dd * rows + half * half_rows, half_rows), half_rows),
                           pl.ds(pl.multiple_of(part * part_cols, part_cols), part_cols)]

        halo = [
            pltpu.make_async_remote_copy(
                src_ref=src.at[0, pl.ds(tok - pad, pad), :], dst_ref=dst, send_sem=halo_send.at[i],
                recv_sem=halo_recv.at[i], device_id=(lax.rem(s + 1, sp), d), device_id_type=MESH)
            for i, (src, dst) in enumerate(((v_hbm, halo_v), (g_hbm, halo_g)))
        ]

        def send_halo():
            @pl.when(s < sp - 1)
            def _():
                for copy in halo:
                    copy.start()

        def z_sends(first, last):
            for k in range(first, last):
                target = nearest(s, sp, k)
                for half in range(2):
                    send(block(half, s), z_sem.at[half, s], (s, d) if sp == 1 else (target, d))

        my_part = s // group
        part_of = [nearest(my_part, parts, k) for k in range(parts)]

        def firsts(half):
            if half == 0:
                return [index(y, along_x(i), core) for i in range(1, xs)]
            return [index(along_y(i), x, core) for i in range(1, ys)]

        def event_own(c):
            part = part_of[c]
            for half in range(2):
                for i in range(group):
                    who = part * group + i
                    if c == 0:
                        if group > 1:
                            @pl.when(who != s)
                            def _():
                                arrived(block(half, who), z_sem.at[half, who])
                    else:
                        arrived(block(half, who), z_sem.at[half, who])
                for target in firsts(half):
                    send(strip(half, d, part), recv_sem.at[half, d, part], (s, target))
            for half in range(2):
                for target in firsts(1 - half):
                    send(strip(half, d, part), recv_sem.at[half, d, part], (s, target))
            for half in range(2):
                send(strip(half, d, part), recv_sem.at[half, d, part], (s, sibling))

        def event_first(c):
            part = part_of[c]
            for half in (1, 0):
                for dd in firsts(half):
                    region, sem = strip(half, dd, part), recv_sem.at[half, dd, part]
                    arrived(region, sem)
                    for target in firsts(1 - half):
                        send(region, sem, (s, target))
                    send(region, sem, (s, sibling))

        def event_second(c):
            part = part_of[c]
            for first in range(max(xs, ys)):
                for second in range(1, max(xs, ys)):
                    for half in range(2):
                        fx, fy = (first, second) if half == 0 else (second, first)
                        if fx >= xs or fy >= ys:
                            continue
                        dd = index(along_y(fy), along_x(fx), core)
                        region, sem = strip(half, dd, part), recv_sem.at[half, dd, part]
                        arrived(region, sem)
                        send(region, sem, (s, sibling))

        def gated_rows(part):
            for copy in loads[part]:
                copy.wait()

            def body(j, carry):
                cs = pl.ds(pl.multiple_of(part * in_cols + j * LANES, LANES), LANES)
                value = v_in[:, cs].astype(F32)
                gate = g_in[:, cs].astype(F32)
                gated[pl.ds(pad, tok), cs] = (value * half_sigmoid(gate)).astype(BF16).astype(F32)
                return carry

            lax.fori_loop(0, in_cols // LANES, body, 0)

        def taps_up():
            for copy in small:
                copy.wait()
            taps_f[...] = taps_in[...].astype(F32)

        def halo_rows():
            @pl.when(s == 0)
            def _():
                gated[pl.ds(0, pad), :] = jnp.zeros((pad, width), F32)

            @pl.when(s > 0)
            def _():
                for copy in halo:
                    copy.wait_recv()

                def body(j, carry):
                    cs = pl.ds(pl.multiple_of(j * LANES, LANES), LANES)
                    value = halo_v[:, cs].astype(F32)
                    gate = halo_g[:, cs].astype(F32)
                    gated[pl.ds(0, pad), cs] = (value * half_sigmoid(gate)).astype(BF16).astype(F32)
                    return carry

                lax.fori_loop(0, blocks, body, 0)

        def mix(row_starts, lo, hi):
            def body(j, carry):
                cs = pl.ds(pl.multiple_of(j * LANES, LANES), LANES)
                for start in row_starts:
                    seen = gated[pl.ds(start, row_chunk + pad), cs]
                    total = None
                    for r in range(8):
                        inner = None
                        length = row_chunk + (8 if r else 0)
                        for q in range(0, pad // 8 + 1):
                            tap = 8 * q + r - lead
                            if 0 <= tap < taps:
                                term = seen[8 * q:8 * q + length] * taps_f[pl.ds(tap, 1), cs]
                                inner = term if inner is None else inner + term
                        if inner is None:
                            continue
                        if r:
                            inner = pltpu.roll(inner, length - r, 0)[:row_chunk]
                        total = inner if total is None else total + inner
                    conv[pl.ds(start, row_chunk), cs] = total.astype(BF16).astype(F32)
                return carry

            lax.fori_loop(lo, hi, body, 0)

        def normalise():
            step = 32 if tok % 32 == 0 else tok

            def body(i, carry):
                rs = pl.ds(pl.multiple_of(i * step, step), step)
                wide = conv[rs, :]
                mean = jnp.sum(wide, axis=1, keepdims=True) * (1.0 / width)
                centered = wide - mean
                variance = jnp.sum(centered * centered, axis=1, keepdims=True) * (1.0 / width)
                scale = lax.rsqrt(variance + EPSILON)
                normed = centered * scale * gain[...] + shift[...]
                act[rs, :] = (normed * half_sigmoid(normed)).astype(BF16)
                return carry

            lax.fori_loop(0, tok // step, body, 0)

        def product(dd, part):
            ks = pl.ds(pl.multiple_of(dd * rows, rows), rows)
            ns = pl.ds(pl.multiple_of(part * part_cols, part_cols), part_cols)
            return ns, jnp.dot(act[:, ks], wall[ks, ns], preferred_element_type=F32)

        def sibling_strip(dd, part):
            for half in range(2):
                arrived(strip(half, dd, part), recv_sem.at[half, dd, part])

        def mm_own(c):
            part = part_of[c]
            sibling_strip(sibling, part)
            if streamed:
                ns, first = product(d, part)
                acc[:, ns] = first
                ns, second = product(sibling, part)
                acc[:, ns] += second

        def mm_rest(c):
            part = part_of[c]

            def body(j, carry):
                xx = lax.rem(x + lax.rem(j, xs), xs)
                yy = lax.rem(y + j // xs, ys)
                theirs = index(yy, xx, 1 - core)
                if streamed:
                    ns, first = product(index(yy, xx, core), part)
                    acc[:, ns] += first
                sibling_strip(theirs, part)
                if streamed:
                    ns, second = product(theirs, part)
                    acc[:, ns] += second
                return carry

            lax.fori_loop(1, xs * ys, body, 0)
            if streamed:
                ns = pl.ds(pl.multiple_of(part * part_cols, part_cols), part_cols)
                out_v[:, ns] = acc[:, ns].astype(BF16)
                copy = pltpu.make_async_copy(out_v.at[:, ns], out_hbm.at[0, :, ns], out_sem.at[c])
                copy.start()
                outs.append(copy)

        outs = []
        early = [start for start in range(0, tok, row_chunk) if start >= pad]
        late = [start for start in range(0, tok, row_chunk) if start < pad]

        compute = [lambda p=p: gated_rows(p) for p in range(in_parts)] + [taps_up]
        quarter = max(1, blocks // 4)
        edges = list(range(0, blocks, quarter)) + [blocks]
        compute += [lambda a=a, b=b: mix(early, a, b) for a, b in zip(edges[:-1], edges[1:])]
        compute += [halo_rows, lambda: mix(late, 0, blocks), normalise]
        events = []
        for c in range(parts + 2):
            if 1 <= c < parts:
                events.append(lambda c=c: event_own(c))
            if 1 <= c <= parts:
                events.append(lambda c=c: event_first(c - 1))
            if c >= 2:
                events.append(lambda c=c: event_second(c - 2))

        z_sends(1, 2)
        event_own(0)
        send_halo()
        z_sends(2, sp)

        relays = []
        for c in range(parts):
            relays.append(("first", c))
            if c + 1 < parts:
                relays.append(("own", c + 1))
            if c >= 1:
                relays.append(("second", c - 1))
        relays.append(("second", parts - 1))
        run = {"own": event_own, "first": event_first, "second": event_second}
        between = {6: 1, 7: 1, 9: 1, 11: 1}
        done = 0
        for number, piece in enumerate(compute):
            piece()
            for _ in range(between.get(number, 0)):
                if done < len(relays):
                    run[relays[done][0]](relays[done][1])
                    done += 1
        pending = [("own", 0)] + relays
        for number, (kind, c) in enumerate(pending):
            if number > done:
                run[kind](c)
            if kind == "own":
                mm_own(c)
            if kind == "second":
                mm_rest(c)

        if not streamed:
            k_step = 2 * LANES
            n_step = 4 * LANES

            def body(i, carry):
                ns = pl.ds(pl.multiple_of(i * n_step, n_step), n_step)
                acc[:, ns] = jnp.zeros((tok, n_step), F32)

                def inner(k, carry):
                    ks = pl.ds(pl.multiple_of(k * k_step, k_step), k_step)
                    acc[:, ns] += jnp.dot(act[:, ks], wall[ks, ns], preferred_element_type=F32)
                    return carry

                lax.fori_loop(0, width // k_step, inner, 0)
                out_v[:, ns] = acc[:, ns].astype(BF16)
                return carry

            lax.fori_loop(0, width // n_step, body, 0)
            copy = pltpu.make_async_copy(out_v, out_hbm.at[0], out_sem.at[0])
            copy.start()
            outs.append(copy)

        for copy in outs:
            copy.wait()
        for copy in sent:
            copy.wait_send()

        @pl.when(s < sp - 1)
        def _():
            for copy in halo:
                copy.wait_send()

    per_half = [(xs, ys), (ys, xs)]
    sends = 2 * (sp - 1)
    for one, two in per_half:
        sends += parts * (one + two - 1) + parts * (one - 1) * two + parts * one * (two - 1)
    scratch = [
        pltpu.VMEM((tok, width), BF16),
        pltpu.VMEM((tok, width), BF16),
        pltpu.VMEM((pad, width), BF16),
        pltpu.VMEM((pad, width), BF16),
        pltpu.VMEM((taps, width), BF16),
        pltpu.VMEM((taps, width), F32),
        pltpu.VMEM((1, width), F32),
        pltpu.VMEM((1, width), F32),
        pltpu.VMEM((pad + tok, width), F32),
        pltpu.VMEM((tok, width), F32),
        pltpu.VMEM((tok, width), BF16),
        pltpu.VMEM((tok, width), F32),
        pltpu.VMEM((tok, width), BF16),
        pltpu.VMEM((dp * rows, sp * cols), BF16),
        pltpu.SemaphoreType.DMA((4 + 2 * in_parts,)),
        pltpu.SemaphoreType.DMA((parts,)),
        pltpu.SemaphoreType.DMA((2,)),
        pltpu.SemaphoreType.DMA((2,)),
        pltpu.SemaphoreType.DMA((sends,)),
        pltpu.SemaphoreType.DMA((2, sp)),
        pltpu.SemaphoreType.DMA((2, dp, parts)),
    ]
    return kernel, scratch


def solution(mesh):
    sp, dp = mesh.shape["sp"], mesh.shape["dp"]
    chips = dp // 2
    xs = max(i for i in range(1, math.isqrt(chips) + 1) if chips % i == 0)
    ys = chips // xs
    parts = math.gcd(sp, max(1, 32 // dp))

    def per_device(value_half, gate_half, conv_taps, norm_gain, norm_shift, out_weight):
        _, tok, width = value_half.shape
        taps = conv_taps.shape[0]
        rows, cols = out_weight.shape
        pad = -(-(taps - 1) // 16) * 16
        kernel, scratch = make_kernel(sp, dp, xs, ys, parts, tok, width, taps, rows, cols, pad)
        return pl.pallas_call(
            kernel,
            out_shape=jax.ShapeDtypeStruct(value_half.shape, BF16),
            in_specs=[pl.BlockSpec(memory_space=pl.ANY)] * 6,
            out_specs=pl.BlockSpec(memory_space=pl.ANY),
            scratch_shapes=scratch,
            compiler_params=pltpu.CompilerParams(
                collective_id=0, has_side_effects=True, vmem_limit_bytes=48 * 1024 * 1024),
        )(value_half, gate_half, conv_taps, norm_gain[None], norm_shift[None], out_weight)

    placed = (P("dp", "sp", None), P("dp", "sp", None), P(), P(), P(), P("dp", "sp"))
    return jax.shard_map(
        per_device, mesh=mesh, in_specs=placed, out_specs=P("dp", "sp", None), check_vma=False
    )
```

```python
import math

import jax
import jax.numpy as jnp
from jax import lax
from jax.experimental import pallas as pl
from jax.experimental.pallas import tpu as pltpu
from jax.sharding import PartitionSpec as P

EPSILON = 1e-06
MESH = pl.DeviceIdType.MESH
F32 = jnp.float32
BF16 = jnp.bfloat16
LANES = 128
BEHIND = {6: 2, 7: 2, 8: 1, 10: 1, 11: 1, 12: 1}


def half_sigmoid(x):
    return 0.5 * jnp.tanh(0.5 * x) + 0.5


def nearest(me, count, k):
    place = jnp.int32(0)
    for here in range(count):
        there = sorted(range(count), key=lambda j: (abs(j - here), j))[k]
        place = place + jnp.where(me == here, there, 0).astype(jnp.int32)
    return place


def make_kernel(sp, dp, xs, ys, parts, tok, width, taps, rows, cols, pad):
    group = sp // parts
    part_cols = group * cols
    half_rows = rows // 2
    blocks = width // LANES
    row_chunk = 128 if tok % 128 == 0 else tok
    lead = pad - (taps - 1)
    in_parts = 4 if blocks % 4 == 0 else 1
    in_cols = width // in_parts
    streamed = rows % LANES == 0

    def kernel(v_hbm, g_hbm, taps_hbm, gain_hbm, shift_hbm, w_hbm, out_hbm,
               v_in, g_in, halo_v, halo_g, taps_in, taps_f, gain, shift, gated, conv, act, acc, out_v, wall,
               in_sem, out_sem, halo_send, halo_recv, send_sem, z_send, z_sem, recv_sem):
        s = lax.axis_index("sp")
        d = lax.axis_index("dp")
        core = lax.rem(d, 2)
        x = lax.rem(d // 2, xs)
        y = d // (2 * xs)

        def index(yy, xx, cc):
            return (yy * xs + xx) * 2 + cc

        sibling = index(y, x, 1 - core)

        def along_x(step):
            return lax.rem(x + step, xs)

        def along_y(step):
            return lax.rem(y + step, ys)

        own = wall.at[pl.ds(pl.multiple_of(d * rows, rows), rows), pl.ds(pl.multiple_of(s * cols, cols), cols)]
        w_copy = pltpu.make_async_copy(w_hbm, own, in_sem.at[0])
        w_copy.start()
        loads = []
        for part in range(in_parts):
            sl = pl.ds(part * in_cols, in_cols)
            pair = (
                pltpu.make_async_copy(v_hbm.at[0, :, sl], v_in.at[:, sl], in_sem.at[4 + 2 * part]),
                pltpu.make_async_copy(g_hbm.at[0, :, sl], g_in.at[:, sl], in_sem.at[5 + 2 * part]),
            )
            loads.append(pair)
            for copy in pair:
                copy.start()
        small = [
            pltpu.make_async_copy(taps_hbm, taps_in, in_sem.at[1]),
            pltpu.make_async_copy(gain_hbm, gain, in_sem.at[2]),
            pltpu.make_async_copy(shift_hbm, shift, in_sem.at[3]),
        ]
        for copy in small:
            copy.start()

        barrier = pltpu.get_barrier_semaphore()
        friends = [(s, sibling)]
        friends += [(s, index(y, along_x(i), core)) for i in range(1, xs)]
        friends += [(s, index(along_y(i), x, core)) for i in range(1, ys)]
        friends += [(lax.rem(s + i, sp), d) for i in range(1, sp)]
        for friend in friends:
            pl.semaphore_signal(barrier, inc=1, device_id=friend, device_id_type=MESH)
        pl.semaphore_wait(barrier, len(friends))
        w_copy.wait()

        sent = []

        def send(region, sem, target):
            copy = pltpu.make_async_remote_copy(
                src_ref=region, dst_ref=region, send_sem=send_sem.at[len(sent)], recv_sem=sem,
                device_id=target, device_id_type=MESH)
            copy.start()
            sent.append(copy)

        def arrived(region, sem):
            pltpu.make_async_remote_copy(
                src_ref=region, dst_ref=region, send_sem=send_sem.at[0], recv_sem=sem,
                device_id=(s, sibling), device_id_type=MESH).wait_recv()

        def block(half, who):
            return wall.at[pl.ds(pl.multiple_of(d * rows + half * half_rows, half_rows), half_rows),
                           pl.ds(pl.multiple_of(who * cols, cols), cols)]

        def strip(half, dd, part):
            return wall.at[pl.ds(pl.multiple_of(dd * rows + half * half_rows, half_rows), half_rows),
                           pl.ds(pl.multiple_of(part * part_cols, part_cols), part_cols)]

        halo = [
            pltpu.make_async_remote_copy(
                src_ref=src.at[0, pl.ds(tok - pad, pad), :], dst_ref=dst, send_sem=halo_send.at[i],
                recv_sem=halo_recv.at[i], device_id=(lax.rem(s + 1, sp), d), device_id_type=MESH)
            for i, (src, dst) in enumerate(((v_hbm, halo_v), (g_hbm, halo_g)))
        ]

        def send_halo():
            @pl.when(s < sp - 1)
            def _():
                for copy in halo:
                    copy.start()

        guarded = []

        def send_if(wanted, region, sem, target):
            copy = pltpu.make_async_remote_copy(
                src_ref=region, dst_ref=region, send_sem=z_send.at[len(guarded)], recv_sem=sem,
                device_id=(target, d), device_id_type=MESH)

            @pl.when(wanted)
            def _():
                copy.start()

            guarded.append((wanted, copy))

        def z_sends():
            for half in range(2):
                send_if(s + 1 < sp, block(half, s), z_sem.at[half, s], lax.rem(s + 1, sp))
                send_if(s > 0, block(half, s), z_sem.at[half, s], lax.rem(s + sp - 1, sp))

        def z_link(k):
            source = nearest(s, sp, k)
            target = jnp.where(source < s, s + 1, s - 1)
            onward = jnp.logical_and(target >= 0, target < sp)
            return source, lax.rem(target + sp, sp), onward

        def z_forward(k):
            source, target, onward = z_link(k)
            for half in range(2):
                @pl.when(onward)
                def _():
                    arrived(block(half, source), z_sem.at[half, source])

                send_if(onward, block(half, source), z_sem.at[half, source], target)

        def z_last(k):
            source, _, onward = z_link(k)

            @pl.when(jnp.logical_not(onward))
            def _():
                for half in range(2):
                    arrived(block(half, source), z_sem.at[half, source])

        my_part = s // group
        part_of = [nearest(my_part, parts, k) for k in range(parts)]

        def firsts(half):
            if half == 0:
                return [index(y, along_x(i), core) for i in range(1, xs)]
            return [index(along_y(i), x, core) for i in range(1, ys)]

        def event_own(c):
            part = part_of[c]
            if group == 1 and c > 0:
                z_last(c)
            for half in range(2):
                for target in firsts(half):
                    send(strip(half, d, part), recv_sem.at[half, d, part], (s, target))
            for half in range(2):
                for target in firsts(1 - half):
                    send(strip(half, d, part), recv_sem.at[half, d, part], (s, target))
            for half in range(2):
                send(strip(half, d, part), recv_sem.at[half, d, part], (s, sibling))

        def event_first(c):
            part = part_of[c]
            for half in (1, 0):
                for dd in firsts(half):
                    region, sem = strip(half, dd, part), recv_sem.at[half, dd, part]
                    arrived(region, sem)
                    for target in firsts(1 - half):
                        send(region, sem, (s, target))
                    send(region, sem, (s, sibling))

        def event_second(c):
            part = part_of[c]
            for first in range(max(xs, ys)):
                for second in range(1, max(xs, ys)):
                    for half in range(2):
                        fx, fy = (first, second) if half == 0 else (second, first)
                        if fx >= xs or fy >= ys:
                            continue
                        dd = index(along_y(fy), along_x(fx), core)
                        region, sem = strip(half, dd, part), recv_sem.at[half, dd, part]
                        arrived(region, sem)
                        send(region, sem, (s, sibling))

        def gated_rows(part):
            for copy in loads[part]:
                copy.wait()

            def body(j, carry):
                cs = pl.ds(pl.multiple_of(part * in_cols + j * LANES, LANES), LANES)
                value = v_in[:, cs].astype(F32)
                gate = g_in[:, cs].astype(F32)
                gated[pl.ds(pad, tok), cs] = (value * half_sigmoid(gate)).astype(BF16).astype(F32)
                return carry

            lax.fori_loop(0, in_cols // LANES, body, 0)

        def taps_up():
            for copy in small:
                copy.wait()
            taps_f[...] = taps_in[...].astype(F32)

        def halo_rows():
            @pl.when(s == 0)
            def _():
                gated[pl.ds(0, pad), :] = jnp.zeros((pad, width), F32)

            @pl.when(s > 0)
            def _():
                for copy in halo:
                    copy.wait_recv()

                def body(j, carry):
                    cs = pl.ds(pl.multiple_of(j * LANES, LANES), LANES)
                    value = halo_v[:, cs].astype(F32)
                    gate = halo_g[:, cs].astype(F32)
                    gated[pl.ds(0, pad), cs] = (value * half_sigmoid(gate)).astype(BF16).astype(F32)
                    return carry

                lax.fori_loop(0, blocks, body, 0)

        def mix(row_starts, lo, hi):
            def body(j, carry):
                cs = pl.ds(pl.multiple_of(j * LANES, LANES), LANES)
                for start in row_starts:
                    seen = gated[pl.ds(start, row_chunk + pad), cs]
                    total = None
                    for r in range(8):
                        inner = None
                        length = row_chunk + (8 if r else 0)
                        for q in range(0, pad // 8 + 1):
                            tap = 8 * q + r - lead
                            if 0 <= tap < taps:
                                term = seen[8 * q:8 * q + length] * taps_f[pl.ds(tap, 1), cs]
                                inner = term if inner is None else inner + term
                        if inner is None:
                            continue
                        if r:
                            inner = pltpu.roll(inner, length - r, 0)[:row_chunk]
                        total = inner if total is None else total + inner
                    conv[pl.ds(start, row_chunk), cs] = total.astype(BF16).astype(F32)
                return carry

            lax.fori_loop(lo, hi, body, 0)

        def normalise():
            step = 32 if tok % 32 == 0 else tok

            def body(i, carry):
                rs = pl.ds(pl.multiple_of(i * step, step), step)
                wide = conv[rs, :]
                mean = jnp.sum(wide, axis=1, keepdims=True) * (1.0 / width)
                centered = wide - mean
                variance = jnp.sum(centered * centered, axis=1, keepdims=True) * (1.0 / width)
                scale = lax.rsqrt(variance + EPSILON)
                normed = centered * scale * gain[...] + shift[...]
                act[rs, :] = (normed * half_sigmoid(normed)).astype(BF16)
                return carry

            lax.fori_loop(0, tok // step, body, 0)

        def product(dd, part):
            ks = pl.ds(pl.multiple_of(dd * rows, rows), rows)
            ns = pl.ds(pl.multiple_of(part * part_cols, part_cols), part_cols)
            return ns, jnp.dot(act[:, ks], wall[ks, ns], preferred_element_type=F32)

        def sibling_strip(dd, part):
            for half in range(2):
                arrived(strip(half, dd, part), recv_sem.at[half, dd, part])

        def mm_own(c):
            part = part_of[c]
            sibling_strip(sibling, part)
            if streamed:
                ns, first = product(d, part)
                acc[:, ns] = first
                ns, second = product(sibling, part)
                acc[:, ns] += second

        def mm_rest(c):
            part = part_of[c]

            def body(j, carry):
                xx = lax.rem(x + lax.rem(j, xs), xs)
                yy = lax.rem(y + j // xs, ys)
                theirs = index(yy, xx, 1 - core)
                if streamed:
                    ns, first = product(index(yy, xx, core), part)
                    acc[:, ns] += first
                sibling_strip(theirs, part)
                if streamed:
                    ns, second = product(theirs, part)
                    acc[:, ns] += second
                return carry

            lax.fori_loop(1, xs * ys, body, 0)
            if streamed:
                ns = pl.ds(pl.multiple_of(part * part_cols, part_cols), part_cols)
                out_v[:, ns] = acc[:, ns].astype(BF16)
                copy = pltpu.make_async_copy(out_v.at[:, ns], out_hbm.at[0, :, ns], out_sem.at[c])
                copy.start()
                outs.append(copy)

        outs = []
        early = [start for start in range(0, tok, row_chunk) if start >= pad]
        late = [start for start in range(0, tok, row_chunk) if start < pad]

        quarter = max(1, blocks // 4)
        edges = list(range(0, blocks, quarter)) + [blocks]
        mixes = list(zip(edges[:-1], edges[1:]))
        plan = []
        z_sends()
        if group > 1:
            send_halo()
            for k in range(1, sp):
                z_forward(k)
                z_last(k)
            event_own(0)
        else:
            event_own(0)
            send_halo()
        plan = [lambda p=p: gated_rows(p) for p in range(in_parts)] + [taps_up]
        plan += [lambda a=a, b=b: mix(early, a, b) for a, b in mixes]
        plan += [halo_rows]
        plan += [lambda a=a, b=b: mix(late, a, b) for a, b in mixes]
        plan += [normalise]
        relays = ["z1", "f0", "o1", "z2", "z3", "f1", "o2", "s0", "f2", "o3", "s1", "f3", "s2", "s3"]
        known = [name for name in relays if int(name[1:]) < (sp if name[0] == "z" else parts)]
        known = [name for name in known if not (name[0] == "z" and group > 1)]
        for k in range(4, sp if group == 1 else 0):
            known.append("z%d" % k)
        for c in range(4, parts):
            known += ["o%d" % c, "f%d" % c, "s%d" % c]
        run = {"z": z_forward, "o": event_own, "f": event_first, "s": event_second}
        behind = BEHIND
        done = 0
        for number, piece in enumerate(plan):
            piece()
            for _ in range(behind.get(number, 0)):
                if done < len(known):
                    run[known[done][0]](int(known[done][1:]))
                    done += 1
        for number, name in enumerate(["o0"] + known):
            kind, c = name[0], int(name[1:])
            if number > done:
                run[kind](c)
            if kind == "o":
                mm_own(c)
            if kind == "s":
                mm_rest(c)

        if not streamed:
            k_step = 2 * LANES
            n_step = 4 * LANES

            def body(i, carry):
                ns = pl.ds(pl.multiple_of(i * n_step, n_step), n_step)
                acc[:, ns] = jnp.zeros((tok, n_step), F32)

                def inner(k, carry):
                    ks = pl.ds(pl.multiple_of(k * k_step, k_step), k_step)
                    acc[:, ns] += jnp.dot(act[:, ks], wall[ks, ns], preferred_element_type=F32)
                    return carry

                lax.fori_loop(0, width // k_step, inner, 0)
                out_v[:, ns] = acc[:, ns].astype(BF16)
                return carry

            lax.fori_loop(0, width // n_step, body, 0)
            copy = pltpu.make_async_copy(out_v, out_hbm.at[0], out_sem.at[0])
            copy.start()
            outs.append(copy)

        for copy in outs:
            copy.wait()
        for copy in sent:
            copy.wait_send()

        for wanted, copy in guarded:
            @pl.when(wanted)
            def _():
                copy.wait_send()

        @pl.when(s < sp - 1)
        def _():
            for copy in halo:
                copy.wait_send()

    per_half = [(xs, ys), (ys, xs)]
    sends = 0
    for one, two in per_half:
        sends += parts * (one + two - 1) + parts * (one - 1) * two + parts * one * (two - 1)
    scratch = [
        pltpu.VMEM((tok, width), BF16),
        pltpu.VMEM((tok, width), BF16),
        pltpu.VMEM((pad, width), BF16),
        pltpu.VMEM((pad, width), BF16),
        pltpu.VMEM((taps, width), BF16),
        pltpu.VMEM((taps, width), F32),
        pltpu.VMEM((1, width), F32),
        pltpu.VMEM((1, width), F32),
        pltpu.VMEM((pad + tok, width), F32),
        pltpu.VMEM((tok, width), F32),
        pltpu.VMEM((tok, width), BF16),
        pltpu.VMEM((tok, width), F32),
        pltpu.VMEM((tok, width), BF16),
        pltpu.VMEM((dp * rows, sp * cols), BF16),
        pltpu.SemaphoreType.DMA((4 + 2 * in_parts,)),
        pltpu.SemaphoreType.DMA((parts,)),
        pltpu.SemaphoreType.DMA((2,)),
        pltpu.SemaphoreType.DMA((2,)),
        pltpu.SemaphoreType.DMA((sends,)),
        pltpu.SemaphoreType.DMA((2 * (sp + 1),)),
        pltpu.SemaphoreType.DMA((2, sp)),
        pltpu.SemaphoreType.DMA((2, dp, parts)),
    ]
    return kernel, scratch


def solution(mesh):
    sp, dp = mesh.shape["sp"], mesh.shape["dp"]
    chips = dp // 2
    xs = max(i for i in range(1, math.isqrt(chips) + 1) if chips % i == 0)
    ys = chips // xs
    parts = math.gcd(sp, max(1, 32 // dp))

    def per_device(value_half, gate_half, conv_taps, norm_gain, norm_shift, out_weight):
        _, tok, width = value_half.shape
        taps = conv_taps.shape[0]
        rows, cols = out_weight.shape
        pad = -(-(taps - 1) // 16) * 16
        kernel, scratch = make_kernel(sp, dp, xs, ys, parts, tok, width, taps, rows, cols, pad)
        return pl.pallas_call(
            kernel,
            out_shape=jax.ShapeDtypeStruct(value_half.shape, BF16),
            in_specs=[pl.BlockSpec(memory_space=pltpu.HBM)] * 6,
            out_specs=pl.BlockSpec(memory_space=pltpu.HBM),
            scratch_shapes=scratch,
            compiler_params=pltpu.CompilerParams(
                collective_id=0, has_side_effects=True, vmem_limit_bytes=63 * 1024 * 1024),
        )(value_half, gate_half, conv_taps, norm_gain[None], norm_shift[None], out_weight)

    placed = (P("dp", "sp", None), P("dp", "sp", None), P(), P(), P(), P("dp", "sp"))
    return jax.shard_map(
        per_device, mesh=mesh, in_specs=placed, out_specs=P("dp", "sp", None), check_vma=False
    )
```

```python
import math

import jax
import jax.numpy as jnp
from jax import lax
from jax.experimental import pallas as pl
from jax.experimental.pallas import tpu as pltpu
from jax.sharding import PartitionSpec as P

EPSILON = 1e-06
MESH = pl.DeviceIdType.MESH
F32 = jnp.float32
BF16 = jnp.bfloat16
LANES = 128
VMEM_LIMIT = 62 * 1024 * 1024
BEHIND = {6: 2, 7: 2, 8: 1, 10: 1, 11: 1, 12: 1}


def half_sigmoid(x):
    return 0.5 * jnp.tanh(0.5 * x) + 0.5


def nearest(me, count, k):
    place = jnp.int32(0)
    for here in range(count):
        there = sorted(range(count), key=lambda j: (abs(j - here), j))[k]
        place = place + jnp.where(me == here, there, 0).astype(jnp.int32)
    return place


def make_kernel(sp, dp, xs, ys, parts, tok, width, taps, rows, cols, pad):
    group = sp // parts
    part_cols = group * cols
    half_rows = rows // 2
    blocks = width // LANES
    row_chunk = 128 if tok % 128 == 0 else tok
    lead = pad - (taps - 1)
    in_parts = 4 if blocks % 4 == 0 else 1
    in_cols = width // in_parts
    streamed = rows % LANES == 0

    def kernel(v_hbm, g_hbm, taps_hbm, gain_hbm, shift_hbm, w_hbm, out_v,
               v_in, g_in, halo_v, halo_g, taps_in, taps_f, gain, shift, gated, conv, act, acc, wall,
               in_sem, halo_send, halo_recv, send_sem, z_send, z_sem, recv_sem):
        s = lax.axis_index("sp")
        d = lax.axis_index("dp")
        core = lax.rem(d, 2)
        x = lax.rem(d // 2, xs)
        y = d // (2 * xs)

        def index(yy, xx, cc):
            return (yy * xs + xx) * 2 + cc

        sibling = index(y, x, 1 - core)

        def along_x(step):
            return lax.rem(x + step, xs)

        def along_y(step):
            return lax.rem(y + step, ys)

        own = wall.at[pl.ds(pl.multiple_of(d * rows, rows), rows), pl.ds(pl.multiple_of(s * cols, cols), cols)]
        w_copy = pltpu.make_async_copy(w_hbm, own, in_sem.at[0])
        w_copy.start()
        loads = []
        for part in range(in_parts):
            sl = pl.ds(part * in_cols, in_cols)
            pair = (
                pltpu.make_async_copy(v_hbm.at[0, :, sl], v_in.at[:, sl], in_sem.at[4 + 2 * part]),
                pltpu.make_async_copy(g_hbm.at[0, :, sl], g_in.at[:, sl], in_sem.at[5 + 2 * part]),
            )
            loads.append(pair)
            for copy in pair:
                copy.start()
        small = [
            pltpu.make_async_copy(taps_hbm, taps_in, in_sem.at[1]),
            pltpu.make_async_copy(gain_hbm, gain, in_sem.at[2]),
            pltpu.make_async_copy(shift_hbm, shift, in_sem.at[3]),
        ]
        for copy in small:
            copy.start()

        barrier = pltpu.get_barrier_semaphore()
        friends = [(s, sibling)]
        friends += [(s, index(y, along_x(i), core)) for i in range(1, xs)]
        friends += [(s, index(along_y(i), x, core)) for i in range(1, ys)]
        friends += [(lax.rem(s + i, sp), d) for i in range(1, sp)]
        for friend in friends:
            pl.semaphore_signal(barrier, inc=1, device_id=friend, device_id_type=MESH)
        pl.semaphore_wait(barrier, len(friends))
        w_copy.wait()

        sent = []

        def send(region, sem, target):
            copy = pltpu.make_async_remote_copy(
                src_ref=region, dst_ref=region, send_sem=send_sem.at[len(sent)], recv_sem=sem,
                device_id=target, device_id_type=MESH)
            copy.start()
            sent.append(copy)

        def arrived(region, sem):
            pltpu.make_async_remote_copy(
                src_ref=region, dst_ref=region, send_sem=send_sem.at[0], recv_sem=sem,
                device_id=(s, sibling), device_id_type=MESH).wait_recv()

        def block(half, who):
            return wall.at[pl.ds(pl.multiple_of(d * rows + half * half_rows, half_rows), half_rows),
                           pl.ds(pl.multiple_of(who * cols, cols), cols)]

        def strip(half, dd, part):
            return wall.at[pl.ds(pl.multiple_of(dd * rows + half * half_rows, half_rows), half_rows),
                           pl.ds(pl.multiple_of(part * part_cols, part_cols), part_cols)]

        halo = [
            pltpu.make_async_remote_copy(
                src_ref=src.at[0, pl.ds(tok - pad, pad), :], dst_ref=dst, send_sem=halo_send.at[i],
                recv_sem=halo_recv.at[i], device_id=(lax.rem(s + 1, sp), d), device_id_type=MESH)
            for i, (src, dst) in enumerate(((v_hbm, halo_v), (g_hbm, halo_g)))
        ]

        def send_halo():
            @pl.when(s < sp - 1)
            def _():
                for copy in halo:
                    copy.start()

        guarded = []

        def send_if(wanted, region, sem, target):
            copy = pltpu.make_async_remote_copy(
                src_ref=region, dst_ref=region, send_sem=z_send.at[len(guarded)], recv_sem=sem,
                device_id=(target, d), device_id_type=MESH)

            @pl.when(wanted)
            def _():
                copy.start()

            guarded.append((wanted, copy))

        def z_sends():
            for half in range(2):
                send_if(s + 1 < sp, block(half, s), z_sem.at[half, s], lax.rem(s + 1, sp))
                send_if(s > 0, block(half, s), z_sem.at[half, s], lax.rem(s + sp - 1, sp))

        def z_link(k):
            source = nearest(s, sp, k)
            target = jnp.where(source < s, s + 1, s - 1)
            onward = jnp.logical_and(target >= 0, target < sp)
            return source, lax.rem(target + sp, sp), onward

        def z_forward(k):
            source, target, onward = z_link(k)
            for half in range(2):
                @pl.when(onward)
                def _():
                    arrived(block(half, source), z_sem.at[half, source])

                send_if(onward, block(half, source), z_sem.at[half, source], target)

        def z_last(k):
            source, _, onward = z_link(k)

            @pl.when(jnp.logical_not(onward))
            def _():
                for half in range(2):
                    arrived(block(half, source), z_sem.at[half, source])

        my_part = s // group
        part_of = [nearest(my_part, parts, k) for k in range(parts)]

        def firsts(half):
            if half == 0:
                return [index(y, along_x(i), core) for i in range(1, xs)]
            return [index(along_y(i), x, core) for i in range(1, ys)]

        def event_own(c):
            part = part_of[c]
            if group == 1 and c > 0:
                z_last(c)
            for half in range(2):
                for target in firsts(half):
                    send(strip(half, d, part), recv_sem.at[half, d, part], (s, target))
            for half in range(2):
                for target in firsts(1 - half):
                    send(strip(half, d, part), recv_sem.at[half, d, part], (s, target))
            for half in range(2):
                send(strip(half, d, part), recv_sem.at[half, d, part], (s, sibling))

        def event_first(c):
            part = part_of[c]
            for half in (1, 0):
                for dd in firsts(half):
                    region, sem = strip(half, dd, part), recv_sem.at[half, dd, part]
                    arrived(region, sem)
                    for target in firsts(1 - half):
                        send(region, sem, (s, target))
                    send(region, sem, (s, sibling))

        def event_second(c):
            part = part_of[c]
            for first in range(max(xs, ys)):
                for second in range(1, max(xs, ys)):
                    for half in range(2):
                        fx, fy = (first, second) if half == 0 else (second, first)
                        if fx >= xs or fy >= ys:
                            continue
                        dd = index(along_y(fy), along_x(fx), core)
                        region, sem = strip(half, dd, part), recv_sem.at[half, dd, part]
                        arrived(region, sem)
                        send(region, sem, (s, sibling))

        def gated_rows(part):
            for copy in loads[part]:
                copy.wait()

            def body(j, carry):
                cs = pl.ds(pl.multiple_of(part * in_cols + j * LANES, LANES), LANES)
                value = v_in[:, cs].astype(F32)
                gate = g_in[:, cs].astype(F32)
                gated[pl.ds(pad, tok), cs] = (value * half_sigmoid(gate)).astype(BF16).astype(F32)
                return carry

            lax.fori_loop(0, in_cols // LANES, body, 0)

        def taps_up():
            for copy in small:
                copy.wait()
            taps_f[...] = taps_in[...].astype(F32)

        def halo_rows():
            @pl.when(s == 0)
            def _():
                gated[pl.ds(0, pad), :] = jnp.zeros((pad, width), F32)

            @pl.when(s > 0)
            def _():
                for copy in halo:
                    copy.wait_recv()

                def body(j, carry):
                    cs = pl.ds(pl.multiple_of(j * LANES, LANES), LANES)
                    value = halo_v[:, cs].astype(F32)
                    gate = halo_g[:, cs].astype(F32)
                    gated[pl.ds(0, pad), cs] = (value * half_sigmoid(gate)).astype(BF16).astype(F32)
                    return carry

                lax.fori_loop(0, blocks, body, 0)

        def mix(row_starts, lo, hi):
            def body(j, carry):
                cs = pl.ds(pl.multiple_of(j * LANES, LANES), LANES)
                for start in row_starts:
                    seen = gated[pl.ds(start, row_chunk + pad), cs]
                    total = None
                    for r in range(8):
                        inner = None
                        length = row_chunk + (8 if r else 0)
                        for q in range(0, pad // 8 + 1):
                            tap = 8 * q + r - lead
                            if 0 <= tap < taps:
                                term = seen[8 * q:8 * q + length] * taps_f[pl.ds(tap, 1), cs]
                                inner = term if inner is None else inner + term
                        if inner is None:
                            continue
                        if r:
                            inner = pltpu.roll(inner, length - r, 0)[:row_chunk]
                        total = inner if total is None else total + inner
                    conv[pl.ds(start, row_chunk), cs] = total.astype(BF16).astype(F32)
                return carry

            lax.fori_loop(lo, hi, body, 0)

        def normalise():
            step = 32 if tok % 32 == 0 else tok

            def body(i, carry):
                rs = pl.ds(pl.multiple_of(i * step, step), step)
                wide = conv[rs, :]
                mean = jnp.sum(wide, axis=1, keepdims=True) * (1.0 / width)
                centered = wide - mean
                variance = jnp.sum(centered * centered, axis=1, keepdims=True) * (1.0 / width)
                scale = lax.rsqrt(variance + EPSILON)
                normed = centered * scale * gain[...] + shift[...]
                act[rs, :] = (normed * half_sigmoid(normed)).astype(BF16)
                return carry

            lax.fori_loop(0, tok // step, body, 0)

        def product(dd, part):
            ks = pl.ds(pl.multiple_of(dd * rows, rows), rows)
            ns = pl.ds(pl.multiple_of(part * part_cols, part_cols), part_cols)
            return ns, jnp.dot(act[:, ks], wall[ks, ns], preferred_element_type=F32)

        def sibling_strip(dd, part):
            for half in range(2):
                arrived(strip(half, dd, part), recv_sem.at[half, dd, part])

        def mm_own(c):
            part = part_of[c]
            sibling_strip(sibling, part)
            if streamed:
                ns, first = product(d, part)
                acc[:, ns] = first
                ns, second = product(sibling, part)
                acc[:, ns] += second

        def mm_rest(c):
            part = part_of[c]

            def body(j, carry):
                xx = lax.rem(x + lax.rem(j, xs), xs)
                yy = lax.rem(y + j // xs, ys)
                theirs = index(yy, xx, 1 - core)
                if streamed:
                    ns, first = product(index(yy, xx, core), part)
                    acc[:, ns] += first
                sibling_strip(theirs, part)
                if streamed:
                    ns, second = product(theirs, part)
                    acc[:, ns] += second
                return carry

            lax.fori_loop(1, xs * ys, body, 0)
            if streamed:
                ns = pl.ds(pl.multiple_of(part * part_cols, part_cols), part_cols)
                out_v[0, :, ns] = acc[:, ns].astype(BF16)

        early = [start for start in range(0, tok, row_chunk) if start >= pad]
        late = [start for start in range(0, tok, row_chunk) if start < pad]

        quarter = max(1, blocks // 4)
        edges = list(range(0, blocks, quarter)) + [blocks]
        mixes = list(zip(edges[:-1], edges[1:]))
        plan = []
        z_sends()
        if group > 1:
            send_halo()
            for k in range(1, sp):
                z_forward(k)
                z_last(k)
            event_own(0)
        else:
            event_own(0)
            send_halo()
        plan = [lambda p=p: gated_rows(p) for p in range(in_parts)] + [taps_up]
        plan += [lambda a=a, b=b: mix(early, a, b) for a, b in mixes]
        plan += [halo_rows]
        plan += [lambda a=a, b=b: mix(late, a, b) for a, b in mixes]
        plan += [normalise]
        relays = ["z1", "f0", "o1", "z2", "z3", "f1", "o2", "s0", "f2", "o3", "s1", "f3", "s2", "s3"]
        known = [name for name in relays if int(name[1:]) < (sp if name[0] == "z" else parts)]
        known = [name for name in known if not (name[0] == "z" and group > 1)]
        for k in range(4, sp if group == 1 else 0):
            known.append("z%d" % k)
        for c in range(4, parts):
            known += ["o%d" % c, "f%d" % c, "s%d" % c]
        run = {"z": z_forward, "o": event_own, "f": event_first, "s": event_second}
        behind = BEHIND
        done = 0
        for number, piece in enumerate(plan):
            piece()
            for _ in range(behind.get(number, 0)):
                if done < len(known):
                    run[known[done][0]](int(known[done][1:]))
                    done += 1
        for number, name in enumerate(["o0"] + known):
            kind, c = name[0], int(name[1:])
            if number > done:
                run[kind](c)
            if kind == "o":
                mm_own(c)
            if kind == "s":
                mm_rest(c)

        if not streamed:
            k_step = 2 * LANES
            n_step = 4 * LANES

            def body(i, carry):
                ns = pl.ds(pl.multiple_of(i * n_step, n_step), n_step)
                acc[:, ns] = jnp.zeros((tok, n_step), F32)

                def inner(k, carry):
                    ks = pl.ds(pl.multiple_of(k * k_step, k_step), k_step)
                    acc[:, ns] += jnp.dot(act[:, ks], wall[ks, ns], preferred_element_type=F32)
                    return carry

                lax.fori_loop(0, width // k_step, inner, 0)
                out_v[0, :, ns] = acc[:, ns].astype(BF16)
                return carry

            lax.fori_loop(0, width // n_step, body, 0)

        for copy in sent:
            copy.wait_send()

        for wanted, copy in guarded:
            @pl.when(wanted)
            def _():
                copy.wait_send()

        @pl.when(s < sp - 1)
        def _():
            for copy in halo:
                copy.wait_send()

    per_half = [(xs, ys), (ys, xs)]
    sends = 0
    for one, two in per_half:
        sends += parts * (one + two - 1) + parts * (one - 1) * two + parts * one * (two - 1)
    scratch = [
        pltpu.VMEM((tok, width), BF16),
        pltpu.VMEM((tok, width), BF16),
        pltpu.VMEM((pad, width), BF16),
        pltpu.VMEM((pad, width), BF16),
        pltpu.VMEM((taps, width), BF16),
        pltpu.VMEM((taps, width), F32),
        pltpu.VMEM((1, width), F32),
        pltpu.VMEM((1, width), F32),
        pltpu.VMEM((pad + tok, width), F32),
        pltpu.VMEM((tok, width), F32),
        pltpu.VMEM((tok, width), BF16),
        pltpu.VMEM((tok, width), F32),
        pltpu.VMEM((dp * rows, sp * cols), BF16),
        pltpu.SemaphoreType.DMA((4 + 2 * in_parts,)),
        pltpu.SemaphoreType.DMA((2,)),
        pltpu.SemaphoreType.DMA((2,)),
        pltpu.SemaphoreType.DMA((sends,)),
        pltpu.SemaphoreType.DMA((2 * (sp + 1),)),
        pltpu.SemaphoreType.DMA((2, sp)),
        pltpu.SemaphoreType.DMA((2, dp, parts)),
    ]
    return kernel, scratch


def solution(mesh):
    sp, dp = mesh.shape["sp"], mesh.shape["dp"]
    chips = dp // 2
    xs = max(i for i in range(1, math.isqrt(chips) + 1) if chips % i == 0)
    ys = chips // xs
    parts = math.gcd(sp, max(1, 32 // dp))

    def per_device(value_half, gate_half, conv_taps, norm_gain, norm_shift, out_weight):
        _, tok, width = value_half.shape
        taps = conv_taps.shape[0]
        rows, cols = out_weight.shape
        pad = -(-(taps - 1) // 16) * 16
        kernel, scratch = make_kernel(sp, dp, xs, ys, parts, tok, width, taps, rows, cols, pad)
        return pl.pallas_call(
            kernel,
            out_shape=pltpu.VMEM(value_half.shape, BF16),
            in_specs=[pl.BlockSpec(memory_space=pltpu.HBM)] * 6,
            out_specs=pl.BlockSpec(memory_space=pltpu.VMEM),
            scratch_shapes=scratch,
            compiler_params=pltpu.CompilerParams(
                collective_id=0, has_side_effects=True, vmem_limit_bytes=VMEM_LIMIT),
        )(value_half, gate_half, conv_taps, norm_gain[None], norm_shift[None], out_weight)

    placed = (P("dp", "sp", None), P("dp", "sp", None), P(), P(), P(), P("dp", "sp"))
    return jax.shard_map(
        per_device, mesh=mesh, in_specs=placed, out_specs=P("dp", "sp", None), check_vma=False
    )
```

```python
import math

import jax
import jax.numpy as jnp
from jax import lax
from jax.experimental import pallas as pl
from jax.experimental.pallas import tpu as pltpu
from jax.sharding import PartitionSpec as P

EPSILON = 1e-06
MESH = pl.DeviceIdType.MESH
F32 = jnp.float32
BF16 = jnp.bfloat16
LANES = 128
VMEM_LIMIT = 62 * 1024 * 1024
ORDER = (
    "x0", "g0", "g1", "g2", "g3", "t0", "e0", "f0", "e1", "z1", "a0", "o1",
    "e2", "y0", "z2", "e3", "f1", "n0", "z3", "v0", "o2", "s0", "h0", "l0",
    "l1", "l2", "l3", "f2", "n1", "o3", "w1", "w2", "u1", "m0", "r0", "s1",
    "m1", "r1", "w3", "f3", "u2", "s2", "m2", "r2", "u3", "m3", "s3", "r3",
)


def half_sigmoid(x):
    return 0.5 * jnp.tanh(0.5 * x) + 0.5


def nearest(me, count, k):
    place = jnp.int32(0)
    for here in range(count):
        there = sorted(range(count), key=lambda j: (abs(j - here), j))[k]
        place = place + jnp.where(me == here, there, 0).astype(jnp.int32)
    return place


def make_kernel(sp, dp, xs, ys, parts, tok, width, taps, rows, cols, pad):
    group = sp // parts
    part_cols = group * cols
    late_rows = rows // 8 // 16 * 16 if group == 1 else 0
    half_rows = (rows - late_rows) // 2
    chips = xs * ys
    blocks = width // LANES
    row_chunk = 128 if tok % 128 == 0 else tok
    lead = pad - (taps - 1)
    in_parts = 4 if blocks % 4 == 0 else 1
    in_cols = width // in_parts
    streamed = rows % LANES == 0

    def kernel(v_hbm, g_hbm, taps_hbm, gain_hbm, shift_hbm, w_hbm, out_v,
               v_in, g_in, halo_v, halo_g, taps_in, taps_f, gain, shift, gated, conv, act, acc, wall,
               in_sem, halo_send, halo_recv, send_sem, z_send, z_sem, recv_sem, late_sem):
        s = lax.axis_index("sp")
        d = lax.axis_index("dp")
        core = lax.rem(d, 2)
        x = lax.rem(d // 2, xs)
        y = d // (2 * xs)

        def index(yy, xx, cc):
            return (yy * xs + xx) * 2 + cc

        sibling = index(y, x, 1 - core)

        def along_x(step):
            return lax.rem(x + step, xs)

        def along_y(step):
            return lax.rem(y + step, ys)

        own = wall.at[pl.ds(pl.multiple_of(d * rows, rows), rows), pl.ds(pl.multiple_of(s * cols, cols), cols)]
        w_copy = pltpu.make_async_copy(w_hbm, own, in_sem.at[0])
        w_copy.start()
        loads = []
        for part in range(in_parts):
            sl = pl.ds(part * in_cols, in_cols)
            pair = (
                pltpu.make_async_copy(v_hbm.at[0, :, sl], v_in.at[:, sl], in_sem.at[4 + 2 * part]),
                pltpu.make_async_copy(g_hbm.at[0, :, sl], g_in.at[:, sl], in_sem.at[5 + 2 * part]),
            )
            loads.append(pair)
            for copy in pair:
                copy.start()
        small = [
            pltpu.make_async_copy(taps_hbm, taps_in, in_sem.at[1]),
            pltpu.make_async_copy(gain_hbm, gain, in_sem.at[2]),
            pltpu.make_async_copy(shift_hbm, shift, in_sem.at[3]),
        ]
        for copy in small:
            copy.start()

        barrier = pltpu.get_barrier_semaphore()
        friends = [(s, sibling)]
        friends += [(s, index(y, along_x(i), core)) for i in range(1, xs)]
        friends += [(s, index(along_y(i), x, core)) for i in range(1, ys)]
        friends += [(lax.rem(s + i, sp), d) for i in range(1, sp)]
        for friend in friends:
            pl.semaphore_signal(barrier, inc=1, device_id=friend, device_id_type=MESH)
        pl.semaphore_wait(barrier, len(friends))
        w_copy.wait()

        sent = []

        def send(region, sem, target):
            copy = pltpu.make_async_remote_copy(
                src_ref=region, dst_ref=region, send_sem=send_sem.at[len(sent)], recv_sem=sem,
                device_id=target, device_id_type=MESH)
            copy.start()
            sent.append(copy)

        def arrived(region, sem):
            pltpu.make_async_remote_copy(
                src_ref=region, dst_ref=region, send_sem=send_sem.at[0], recv_sem=sem,
                device_id=(s, sibling), device_id_type=MESH).wait_recv()

        def block(half, who):
            return wall.at[pl.ds(pl.multiple_of(d * rows + half * half_rows, 16), half_rows),
                           pl.ds(pl.multiple_of(who * cols, cols), cols)]

        def strip(half, dd, part):
            return wall.at[pl.ds(pl.multiple_of(dd * rows + half * half_rows, 16), half_rows),
                           pl.ds(pl.multiple_of(part * part_cols, part_cols), part_cols)]

        halo = [
            pltpu.make_async_remote_copy(
                src_ref=src.at[0, pl.ds(tok - pad, pad), :], dst_ref=dst, send_sem=halo_send.at[i],
                recv_sem=halo_recv.at[i], device_id=(lax.rem(s + 1, sp), d), device_id_type=MESH)
            for i, (src, dst) in enumerate(((v_hbm, halo_v), (g_hbm, halo_g)))
        ]

        def send_halo(i):
            @pl.when(s < sp - 1)
            def _():
                halo[i].start()

        guarded = []

        def send_if(wanted, region, sem, target, column=None):
            copy = pltpu.make_async_remote_copy(
                src_ref=region, dst_ref=region, send_sem=z_send.at[len(guarded)], recv_sem=sem,
                device_id=(target, d if column is None else column), device_id_type=MESH)

            @pl.when(wanted)
            def _():
                copy.start()

            guarded.append((wanted, copy))

        def z_sends():
            for half in range(2):
                send_if(s + 1 < sp, block(half, s), z_sem.at[half, s], lax.rem(s + 1, sp))
                send_if(s > 0, block(half, s), z_sem.at[half, s], lax.rem(s + sp - 1, sp))

        def z_link(k):
            source = nearest(s, sp, k)
            target = jnp.where(source < s, s + 1, s - 1)
            onward = jnp.logical_and(target >= 0, target < sp)
            return source, lax.rem(target + sp, sp), onward

        def z_forward(k):
            source, target, onward = z_link(k)
            for half in range(2):
                @pl.when(onward)
                def _():
                    arrived(block(half, source), z_sem.at[half, source])

                send_if(onward, block(half, source), z_sem.at[half, source], target)

        def z_last(k):
            source, _, onward = z_link(k)

            @pl.when(jnp.logical_not(onward))
            def _():
                for half in range(2):
                    arrived(block(half, source), z_sem.at[half, source])

        my_part = s // group
        part_of = [nearest(my_part, parts, k) for k in range(parts)]

        def firsts(half):
            if half == 0:
                return [index(y, along_x(i), core) for i in range(1, xs)]
            return [index(along_y(i), x, core) for i in range(1, ys)]

        def event_own(c):
            part = part_of[c]
            if group == 1 and c > 0:
                z_last(c)
            for half in range(2):
                for target in firsts(half):
                    send(strip(half, d, part), recv_sem.at[half, d, part], (s, target))
            for half in range(2):
                for target in firsts(1 - half):
                    send(strip(half, d, part), recv_sem.at[half, d, part], (s, target))
            for half in range(2):
                send(strip(half, d, part), recv_sem.at[half, d, part], (s, sibling))

        def event_first(c):
            part = part_of[c]
            for half in (1, 0):
                for dd in firsts(half):
                    region, sem = strip(half, dd, part), recv_sem.at[half, dd, part]
                    arrived(region, sem)
                    for target in firsts(1 - half):
                        send(region, sem, (s, target))
                    send(region, sem, (s, sibling))

        def event_second(c):
            part = part_of[c]
            for first in range(max(xs, ys)):
                for second in range(1, max(xs, ys)):
                    for half in range(2):
                        fx, fy = (first, second) if half == 0 else (second, first)
                        if fx >= xs or fy >= ys:
                            continue
                        dd = index(along_y(fy), along_x(fx), core)
                        region, sem = strip(half, dd, part), recv_sem.at[half, dd, part]
                        arrived(region, sem)
                        send(region, sem, (s, sibling))

        def late_strip(dd, who):
            return wall.at[pl.ds(pl.multiple_of(dd * rows + 2 * half_rows, 16), late_rows),
                           pl.ds(pl.multiple_of(who * cols, cols), cols)]

        def mine(i):
            return index(along_y(i // xs), along_x(i % xs), core)

        def late_send(dd, target):
            send(late_strip(dd, s), late_sem.at[dd, s], (s, target))

        def late_x():
            for i in range(1, xs):
                late_send(d, mine(i))

        def late_y():
            for i in range(xs):
                if i:
                    arrived(late_strip(mine(i), s), late_sem.at[mine(i), s])
                for j in range(1, ys):
                    late_send(mine(i), index(along_y(j), x, core))

        def late_z():
            for i in range(chips):
                dd = mine(i)
                if i >= xs:
                    arrived(late_strip(dd, s), late_sem.at[dd, s])
                send_if(s + 1 < sp, late_strip(dd, s), late_sem.at[dd, s], lax.rem(s + 1, sp))
                send_if(s > 0, late_strip(dd, s), late_sem.at[dd, s], lax.rem(s + sp - 1, sp))
                late_send(dd, sibling)

        def late_forward(k):
            source, target, onward = z_link(k)
            for i in range(chips):
                region, sem = late_strip(mine(i), source), late_sem.at[mine(i), source]

                @pl.when(onward)
                def _():
                    arrived(region, sem)

                send_if(onward, region, sem, target)
                send_if(onward, region, sem, s, sibling)

        def late_last(k):
            source, _, onward = z_link(k)
            ended = jnp.logical_not(onward)
            for i in range(chips):
                region, sem = late_strip(mine(i), source), late_sem.at[mine(i), source]

                @pl.when(ended)
                def _():
                    arrived(region, sem)

                send_if(ended, region, sem, s, sibling)

        def gated_rows(part):
            for copy in loads[part]:
                copy.wait()

            def body(j, carry):
                cs = pl.ds(pl.multiple_of(part * in_cols + j * LANES, LANES), LANES)
                value = v_in[:, cs].astype(F32)
                gate = g_in[:, cs].astype(F32)
                gated[pl.ds(pad, tok), cs] = (value * half_sigmoid(gate)).astype(BF16).astype(F32)
                return carry

            lax.fori_loop(0, in_cols // LANES, body, 0)

        def taps_up():
            for copy in small:
                copy.wait()
            taps_f[...] = taps_in[...].astype(F32)

        def halo_rows():
            @pl.when(s == 0)
            def _():
                gated[pl.ds(0, pad), :] = jnp.zeros((pad, width), F32)

            @pl.when(s > 0)
            def _():
                for copy in halo:
                    copy.wait_recv()

                def body(j, carry):
                    cs = pl.ds(pl.multiple_of(j * LANES, LANES), LANES)
                    value = halo_v[:, cs].astype(F32)
                    gate = halo_g[:, cs].astype(F32)
                    gated[pl.ds(0, pad), cs] = (value * half_sigmoid(gate)).astype(BF16).astype(F32)
                    return carry

                lax.fori_loop(0, blocks, body, 0)

        def mix(row_starts, lo, hi):
            def body(j, carry):
                cs = pl.ds(pl.multiple_of(j * LANES, LANES), LANES)
                for start in row_starts:
                    seen = gated[pl.ds(start, row_chunk + pad), cs]
                    total = None
                    for r in range(8):
                        inner = None
                        length = row_chunk + (8 if r else 0)
                        for q in range(0, pad // 8 + 1):
                            tap = 8 * q + r - lead
                            if 0 <= tap < taps:
                                term = seen[8 * q:8 * q + length] * taps_f[pl.ds(tap, 1), cs]
                                inner = term if inner is None else inner + term
                        if inner is None:
                            continue
                        if r:
                            inner = pltpu.roll(inner, length - r, 0)[:row_chunk]
                        total = inner if total is None else total + inner
                    conv[pl.ds(start, row_chunk), cs] = total.astype(BF16).astype(F32)
                return carry

            lax.fori_loop(lo, hi, body, 0)

        def normalise(low, high):
            step = math.gcd(32, row_chunk)

            def body(i, carry):
                rs = pl.ds(pl.multiple_of(i * step, step), step)
                wide = conv[rs, :]
                mean = jnp.sum(wide, axis=1, keepdims=True) * (1.0 / width)
                centered = wide - mean
                variance = jnp.sum(centered * centered, axis=1, keepdims=True) * (1.0 / width)
                scale = lax.rsqrt(variance + EPSILON)
                normed = centered * scale * gain[...] + shift[...]
                act[rs, :] = (normed * half_sigmoid(normed)).astype(BF16)
                return carry

            lax.fori_loop(low // step, high // step, body, 0)

        def product(dd, part):
            ks = pl.ds(pl.multiple_of(dd * rows, rows), rows)
            ns = pl.ds(pl.multiple_of(part * part_cols, part_cols), part_cols)
            return ns, jnp.dot(act[:, ks], wall[ks, ns], preferred_element_type=F32)

        def sibling_strip(dd, part):
            for half in range(2):
                arrived(strip(half, dd, part), recv_sem.at[half, dd, part])
            if late_rows:
                arrived(late_strip(dd, part), late_sem.at[dd, part])

        def mm_own(c):
            part = part_of[c]
            sibling_strip(sibling, part)
            if streamed:
                ns, first = product(d, part)
                acc[:, ns] = first
                ns, second = product(sibling, part)
                acc[:, ns] += second

        def mm_rest(c):
            part = part_of[c]

            def body(j, carry):
                xx = lax.rem(x + lax.rem(j, xs), xs)
                yy = lax.rem(y + j // xs, ys)
                theirs = index(yy, xx, 1 - core)
                if streamed:
                    ns, first = product(index(yy, xx, core), part)
                    acc[:, ns] += first
                sibling_strip(theirs, part)
                if streamed:
                    ns, second = product(theirs, part)
                    acc[:, ns] += second
                return carry

            lax.fori_loop(1, xs * ys, body, 0)
            if streamed:
                ns = pl.ds(pl.multiple_of(part * part_cols, part_cols), part_cols)
                out_v[0, :, ns] = acc[:, ns].astype(BF16)

        early = [start for start in range(0, tok, row_chunk) if start >= pad]
        late = [start for start in range(0, tok, row_chunk) if start < pad]

        edges = [blocks * i // 4 for i in range(5)]
        z_sends()
        if group > 1:
            send_halo(0)
            for k in range(1, sp):
                z_forward(k)
                z_last(k)
            event_own(0)
        else:
            event_own(0)
            send_halo(0)
        run = {
            "g": (gated_rows, 0, in_parts),
            "t": (lambda c: taps_up(), 0, 1),
            "e": (lambda c: mix(early, edges[c], edges[c + 1]), 0, 4),
            "h": (lambda c: halo_rows(), 0, 1),
            "l": (lambda c: mix(late, edges[c], edges[c + 1]), 0, 4),
            "n": (lambda c: normalise(*((late[-1] + row_chunk, tok), (0, late[-1] + row_chunk))[c]), 0, 2),
            "z": (z_forward, 1, sp if group == 1 else 0),
            "o": (event_own, 1, parts),
            "f": (event_first, 0, parts),
            "s": (event_second, 0, parts),
            "a": (lambda c: send_halo(1), 0, 1),
            "x": (lambda c: late_x(), 0, 1 if late_rows else 0),
            "y": (lambda c: late_y(), 0, 1 if late_rows else 0),
            "v": (lambda c: late_z(), 0, 1 if late_rows else 0),
            "w": (late_forward, 1, sp if late_rows else 0),
            "u": (late_last, 1, sp if late_rows else 0),
            "m": (mm_own, 0, parts),
            "r": (mm_rest, 0, parts),
        }
        order = list(ORDER)
        for c in range(max(sp, parts)):
            order += [kind + str(c) for kind in "zowufsmr" if kind + str(c) not in order]
        for name in order:
            act_on, low, high = run[name[0]]
            if low <= int(name[1:]) < high:
                act_on(int(name[1:]))

        if not streamed:
            k_step = 2 * LANES
            n_step = 4 * LANES

            def body(i, carry):
                ns = pl.ds(pl.multiple_of(i * n_step, n_step), n_step)
                acc[:, ns] = jnp.zeros((tok, n_step), F32)

                def inner(k, carry):
                    ks = pl.ds(pl.multiple_of(k * k_step, k_step), k_step)
                    acc[:, ns] += jnp.dot(act[:, ks], wall[ks, ns], preferred_element_type=F32)
                    return carry

                lax.fori_loop(0, width // k_step, inner, 0)
                out_v[0, :, ns] = acc[:, ns].astype(BF16)
                return carry

            lax.fori_loop(0, width // n_step, body, 0)

        for copy in sent:
            copy.wait_send()

        for wanted, copy in guarded:
            @pl.when(wanted)
            def _():
                copy.wait_send()

        @pl.when(s < sp - 1)
        def _():
            for copy in halo:
                copy.wait_send()

    per_half = [(xs, ys), (ys, xs)]
    sends = xs - 1 + xs * (ys - 1) + chips if late_rows else 0
    for one, two in per_half:
        sends += parts * (one + two - 1) + parts * (one - 1) * two + parts * one * (two - 1)
    scratch = [
        pltpu.VMEM((tok, width), BF16),
        pltpu.VMEM((tok, width), BF16),
        pltpu.VMEM((pad, width), BF16),
        pltpu.VMEM((pad, width), BF16),
        pltpu.VMEM((taps, width), BF16),
        pltpu.VMEM((taps, width), F32),
        pltpu.VMEM((1, width), F32),
        pltpu.VMEM((1, width), F32),
        pltpu.VMEM((pad + tok, width), F32),
        pltpu.VMEM((tok, width), F32),
        pltpu.VMEM((tok, width), BF16),
        pltpu.VMEM((tok, width), F32),
        pltpu.VMEM((dp * rows, sp * cols), BF16),
        pltpu.SemaphoreType.DMA((4 + 2 * in_parts,)),
        pltpu.SemaphoreType.DMA((2,)),
        pltpu.SemaphoreType.DMA((2,)),
        pltpu.SemaphoreType.DMA((sends,)),
        pltpu.SemaphoreType.DMA((2 * (sp + 1) + chips * (3 * sp - 1),)),
        pltpu.SemaphoreType.DMA((2, sp)),
        pltpu.SemaphoreType.DMA((2, dp, parts)),
        pltpu.SemaphoreType.DMA((dp, sp) if late_rows else (1, 1)),
    ]
    return kernel, scratch


def solution(mesh):
    sp, dp = mesh.shape["sp"], mesh.shape["dp"]
    chips = dp // 2
    xs = max(i for i in range(1, math.isqrt(chips) + 1) if chips % i == 0)
    ys = chips // xs
    parts = math.gcd(sp, max(1, 32 // dp))

    def per_device(value_half, gate_half, conv_taps, norm_gain, norm_shift, out_weight):
        _, tok, width = value_half.shape
        taps = conv_taps.shape[0]
        rows, cols = out_weight.shape
        pad = -(-(taps - 1) // 16) * 16
        kernel, scratch = make_kernel(sp, dp, xs, ys, parts, tok, width, taps, rows, cols, pad)
        return pl.pallas_call(
            kernel,
            out_shape=pltpu.VMEM(value_half.shape, BF16),
            in_specs=[pl.BlockSpec(memory_space=pltpu.HBM)] * 6,
            out_specs=pl.BlockSpec(memory_space=pltpu.VMEM),
            scratch_shapes=scratch,
            compiler_params=pltpu.CompilerParams(
                collective_id=0, has_side_effects=True, vmem_limit_bytes=VMEM_LIMIT),
        )(value_half, gate_half, conv_taps, norm_gain[None], norm_shift[None], out_weight)

    placed = (P("dp", "sp", None), P("dp", "sp", None), P(), P(), P(), P("dp", "sp"))
    return jax.shard_map(
        per_device, mesh=mesh, in_specs=placed, out_specs=P("dp", "sp", None), check_vma=False
    )
```
